32 devices in a mesh: sp: 16 (over z, y, x), tp: 2 (over core).
Axes of the slice: x: 2, y: 2, z: 4, core: 2. Of those that a mesh axis runs over, the one named last changes fastest.
Arguments:
- mixer_in: bfloat16 [8192, 1024], P('sp', 'tp'), may hold values from -6 to 6
- residual: bfloat16 [8192, 2048], P(('sp', 'tp')), may hold values from -6 to 6
- decay_real: float32 [64, 64], P('tp'), may hold values from -2 to 0, as said below
- decay_imag: float32 [64, 64], P('tp'), may hold values from 1 to 200
- log_step: float32 [64], P('tp'), may hold values from -3.9 to -2.5
- in_real: float32 [64, 64, 16], P('tp'), may hold values from -1 to 1
- in_imag: float32 [64, 64, 16], P('tp'), may hold values from -1 to 1
- output_real: float32 [64, 16, 64], P('tp'), may hold values from -0.5 to 0.5
- output_imaginary: float32 [64, 16, 64], P('tp'), may hold values from -0.5 to 0.5
- skip: float32 [1024], P('tp'), may hold values from -4 to 4
- out_proj: bfloat16 [1024, 2048], P('tp'), may hold values from -0.1875 to 0.1875
- norm_gain: float32 [2048], replicated, may hold values from 0.1 to 1.9
- w_gate: bfloat16 [2048, 5632], P('sp', 'tp'), may hold values from -0.125 to 0.125
- w_up: bfloat16 [2048, 5632], P('sp', 'tp'), may hold values from -0.125 to 0.125
- w_down: bfloat16 [5632, 2048], P('tp', 'sp'), may hold values from -0.078125 to 0.078125
Outputs:
- output: bfloat16 [8192, 2048], P(('sp', 'tp'))
The draws below stay inside these ranges and needn't reach their ends.
Inputs may be any that keep to these rules, and one draw needn't show every extreme that they name: `decay_real`: every entry is negative.
All inputs are finite; a program needn't handle non-finite values.
Results may differ from the reference program's by a relative error of at most 0.02.
Values may be sent and summed in bfloat16 or wider, within the bound.
A program may use at most 128 MiB of HBM per device.

```python
import jax
import jax.numpy as jnp
from jax import lax

D = 2048
CH = 1024
GROUP = 16
STATE = 64
FF = 5632
TOK_DEV = 512
GROUPS = 64
TOKENS = 8192
CH_DEV = 512
FF_DEV = 2816
N_SP = 16


def draw_decay_real(key, part):
    slow_key, rate_key = jax.random.split(jax.random.fold_in(key, 11))
    slow = jax.random.bernoulli(slow_key, 0.5, (GROUPS, 1))
    mixing = jax.random.uniform(rate_key, (GROUPS, STATE), jnp.float32)
    slow_rate = 5.0 / TOKENS * jnp.exp(mixing * jnp.log(5.0))
    fast_rate = 0.6 * jnp.exp(mixing * jnp.log(2.0))
    return -jnp.where(slow, slow_rate, fast_rate)


def level_of(own_key, extent, shards, low, high):
    level = 1.0
    for position, parts in shards:
        heights = jax.random.uniform(jax.random.fold_in(jax.random.fold_in(own_key, 6), position), (parts,), jnp.float32, low / len(shards), high / len(shards))
        level = level * jnp.repeat(jnp.exp(heights), extent[position] // parts).reshape((-1,) + (1,) * (len(extent) - 1 - position))
    return level


def normal_values(key, shape, scale, bound, cuts=(), dtype=jnp.bfloat16):
    loudness = level_of(key, shape, cuts, -0.22, 0.18) if cuts else 1.0
    entries = jax.random.normal(key, shape, jnp.float32) * scale * loudness
    return jnp.minimum(jnp.maximum(entries, -bound), bound).astype(dtype)


def setup_inputs(seed: int = 0) -> dict:
    key_list = jax.random.split(jax.random.key(seed), 16)
    return {
        "mixer_in": normal_values(key_list[0], (TOKENS, CH), 1.0, 6.0, ((0, 16), (1, 2))),
        "residual": normal_values(key_list[1], (TOKENS, D), 1.0, 6.0, ((0, 32),)),
        "decay_real": draw_decay_real(jax.random.fold_in(key_list[15], 71), 0),
        "decay_imag": jnp.clip(1.0 + 199.0 * jax.random.uniform(key_list[3], (GROUPS, STATE), jnp.float32) ** level_of(key_list[3], (GROUPS, STATE), ((0, 2),), -0.2, 0.2), 1.0, 200.0),
        "log_step": jnp.clip(-3.9 + 1.4000001 * jax.random.uniform(key_list[4], (GROUPS,), jnp.float32) ** level_of(key_list[4], (GROUPS,), ((0, 2),), -0.2, 0.2), -3.9, -2.5),
        "in_real": normal_values(key_list[5], (GROUPS, STATE, GROUP), (2 * GROUP) ** -0.5, 1.0, ((0, 2),), jnp.float32),
        "in_imag": normal_values(key_list[6], (GROUPS, STATE, GROUP), (2 * GROUP) ** -0.5, 1.0, ((0, 2),), jnp.float32),
        "output_real": normal_values(key_list[7], (GROUPS, GROUP, STATE), (2 * STATE) ** -0.5, 0.5, ((0, 2),), jnp.float32),
        "output_imaginary": normal_values(key_list[8], (GROUPS, GROUP, STATE), (2 * STATE) ** -0.5, 0.5, ((0, 2),), jnp.float32),
        "skip": normal_values(key_list[9], (CH,), 1.0, 4.0, ((0, 2),), jnp.float32),
        "out_proj": normal_values(key_list[10], (CH, D), CH ** -0.5, 0.1875, ((0, 2),)),
        "norm_gain": jnp.clip(1.0 + 0.18 * jax.random.normal(key_list[11], (D,), jnp.float32), 0.1, 1.9),
        "w_gate": normal_values(key_list[12], (D, FF), D ** -0.5, 0.125, ((0, 16), (1, 2))),
        "w_up": normal_values(key_list[13], (D, FF), D ** -0.5, 0.125, ((0, 16), (1, 2))),
        "w_down": normal_values(key_list[14], (FF, D), FF ** -0.5, 0.078125, ((0, 2), (1, 16))),
    }


def discrete(decay_real, decay_imag, log_step, in_real, in_imag):
    step_size = jnp.exp(log_step)[:, None]
    magnitude = jnp.exp(decay_real * step_size)
    angle = decay_imag * step_size
    power_re = magnitude * jnp.cos(angle)
    power_im = magnitude * jnp.sin(angle)
    denom = decay_real * decay_real + decay_imag * decay_imag
    ratio_re = ((power_re - 1.0) * decay_real + power_im * decay_imag) / denom
    ratio_im = (power_im * decay_real - (power_re - 1.0) * decay_imag) / denom
    drive_re = ratio_re[..., None] * in_real - ratio_im[..., None] * in_imag
    drive_im = ratio_re[..., None] * in_imag + ratio_im[..., None] * in_real
    return (power_re, power_im, drive_re, drive_im)

def combine(earlier, later):
    ar1, ai1, br1, bi1 = earlier
    ar2, ai2, br2, bi2 = later
    return (ar2 * ar1 - ai2 * ai1, ar2 * ai1 + ai2 * ar1, ar2 * br1 - ai2 * bi1 + br2, ar2 * bi1 + ai2 * br1 + bi2)

def block_sum(left, right, width):
    summed = jnp.zeros((left.shape[0], right.shape[1]), jnp.float32)
    for index in range(left.shape[1] // width):
        partial_value = jnp.dot(left[:, index * width:(index + 1) * width], right[index * width:(index + 1) * width], preferred_element_type=jnp.float32).astype(jnp.bfloat16)
        summed = summed + lax.optimization_barrier(partial_value).astype(jnp.float32)
    return summed.astype(jnp.bfloat16)

def reference(mixer_in, residual, decay_real, decay_imag, log_step, in_real, in_imag, output_real, output_imaginary, skip, out_proj, norm_gain, w_gate, w_up, w_down):
    highest_precision = lax.Precision.HIGHEST
    power_re, power_im, bar_re, bar_im = discrete(decay_real, decay_imag, log_step, in_real, in_imag)
    groups, states = decay_real.shape
    signal = mixer_in.astype(jnp.float32).reshape(N_SP, TOK_DEV, groups, GROUP)
    group_skip_gain = skip.reshape(groups, GROUP)

    def advance(carry, block_range):
        hold_re, hold_im = carry
        drive_re = jnp.einsum('tgc,gpc->tgp', block_range, bar_re, precision=highest_precision)
        drive_im = jnp.einsum('tgc,gpc->tgp', block_range, bar_im, precision=highest_precision)
        a_re = jnp.broadcast_to(power_re[None], drive_re.shape)
        a_im = jnp.broadcast_to(power_im[None], drive_re.shape)
        pw_re, pw_im, state_real, state_imaginary = lax.associative_scan(combine, (a_re, a_im, drive_re, drive_im), axis=0)
        state_real = state_real + pw_re * hold_re[None] - pw_im * hold_im[None]
        state_imaginary = state_imaginary + pw_re * hold_im[None] + pw_im * hold_re[None]
        mixed_before_norm = jnp.einsum('uzl,zhl->uzh', state_real, output_real, precision=highest_precision) - jnp.einsum('uzl,zhl->uzh', state_imaginary, output_imaginary, precision=highest_precision) + group_skip_gain[None] * block_range
        return ((state_real[-1], state_imaginary[-1]), mixed_before_norm.reshape(TOK_DEV, groups * GROUP))
    zero_state = jnp.zeros((groups, states), jnp.float32)
    _, mixed_all = lax.scan(advance, (zero_state, zero_state), signal)
    activated = jax.nn.gelu(mixed_all).astype(jnp.bfloat16)
    res_blocks = residual.reshape(N_SP, TOK_DEV, residual.shape[1])

    def finish(pair):
        act_rows, res_rows = pair
        mixed = block_sum(act_rows, out_proj, CH_DEV)
        carried = res_rows.astype(jnp.float32) + mixed.astype(jnp.float32)
        scale = lax.rsqrt(lax.optimization_barrier(jnp.mean(carried * carried, axis=-1, keepdims=True)) + 1e-06)
        normed = (carried * scale * norm_gain).astype(jnp.bfloat16)
        gate = jnp.dot(normed, w_gate, preferred_element_type=jnp.float32)
        up = jnp.dot(normed, w_up, preferred_element_type=jnp.float32)
        hidden = (jax.nn.silu(gate) * up).astype(jnp.bfloat16)
        down = block_sum(hidden, w_down, FF_DEV)
        return (carried + 0.5 * down.astype(jnp.float32)).astype(jnp.bfloat16)
    result = lax.map(finish, (activated, res_blocks))
    return result.reshape(TOKENS, residual.shape[1])
```

```python
import functools

import jax
import jax.numpy as jnp
from jax import lax
from jax.experimental import pallas as pl
from jax.experimental.pallas import tpu as pltpu
from jax.sharding import Mesh
from jax.sharding import PartitionSpec as P

F32 = jnp.float32
BF16 = jnp.bfloat16
SP = ("h", "u", "m", "v")
PEERS = ("u", "v")
GATHER = 8
CHUNKS = 8


def discrete(decay_real, decay_imag, log_step, in_real, in_imag):
    step_size = jnp.exp(log_step)[:, None]
    magnitude = jnp.exp(decay_real * step_size)
    angle = decay_imag * step_size
    power_re = magnitude * jnp.cos(angle)
    power_im = magnitude * jnp.sin(angle)
    denom = decay_real * decay_real + decay_imag * decay_imag
    ratio_re = ((power_re - 1.0) * decay_real + power_im * decay_imag) / denom
    ratio_im = (power_im * decay_real - (power_re - 1.0) * decay_imag) / denom
    drive_re = ratio_re[..., None] * in_real - ratio_im[..., None] * in_imag
    drive_im = ratio_re[..., None] * in_imag + ratio_im[..., None] * in_real
    return (power_re, power_im, drive_re, drive_im)


def spread(matrix):
    groups, rows, columns = matrix.shape
    eye = jnp.eye(GATHER, dtype=F32)[None, :, None, :, None]
    pieces = matrix.reshape(groups // GATHER, GATHER, rows, 1, columns)
    return (eye * pieces).reshape(groups // GATHER, GATHER * rows, GATHER * columns)


def cmul(ar, ai, br, bi):
    return ar * br - ai * bi, ar * bi + ai * br


def cpow(ar, ai, count):
    result = None
    while count:
        if count & 1:
            result = (ar, ai) if result is None else cmul(*result, ar, ai)
        count >>= 1
        if count:
            ar, ai = cmul(ar, ai, ar, ai)
    return result


def scan_ends(x_ref, b_ref, a_ref, s_ref, e_ref, work):
    rows, width = work.shape
    half = width // 2
    work[...] = jnp.dot(x_ref[...], b_ref[0], preferred_element_type=F32)
    ar, ai = a_ref[0, 0:1, :], a_ref[0, 1:2, :]
    br = jnp.broadcast_to(ar, (CHUNKS, half))
    bi = jnp.broadcast_to(ai, (CHUNKS, half))

    def step(index, state):
        sr, si = state
        at = pl.ds(pl.multiple_of(index * CHUNKS, CHUNKS), CHUNKS)
        nr, ni = cmul(br, bi, sr, si)
        return nr + work[at, :half], ni + work[at, half:]

    zero = jnp.zeros((CHUNKS, half), F32)
    sr, si = lax.fori_loop(0, rows // CHUNKS, step, (zero, zero), unroll=8)
    s_ref[0, :, :half] = sr
    s_ref[0, :, half:] = si
    lr, li = cpow(ar, ai, rows // CHUNKS)
    er, ei = sr[0:1], si[0:1]
    for chunk in range(1, CHUNKS):
        er, ei = cmul(lr, li, er, ei)
        er, ei = er + sr[chunk:chunk + 1], ei + si[chunk:chunk + 1]
    e_ref[0, :, :half] = er
    e_ref[0, :, half:] = ei


def scan_outputs(me_ref, x_ref, b_ref, c_ref, a_ref, s_ref, g_ref, k_ref, o_ref, work):
    rows, width = work.shape
    half = width // 2
    work[...] = jnp.dot(x_ref[...], b_ref[0], preferred_element_type=F32)
    ar, ai = a_ref[0, 0:1, :], a_ref[0, 1:2, :]
    lr, li = cpow(ar, ai, rows // CHUNKS)
    tr, ti = cpow(lr, li, CHUNKS)
    me = me_ref[0]
    hr = jnp.zeros((1, half), F32)
    hi = hr
    for device in range(g_ref.shape[1] - 1):
        nr, ni = cmul(tr, ti, hr, hi)
        nr = nr + g_ref[0, device:device + 1, :half]
        ni = ni + g_ref[0, device:device + 1, half:]
        hr, hi = jnp.where(device < me, nr, hr), jnp.where(device < me, ni, hi)
    starts_r, starts_i = [hr], [hi]
    for chunk in range(CHUNKS - 1):
        nr, ni = cmul(lr, li, hr, hi)
        hr = nr + s_ref[0, chunk:chunk + 1, :half]
        hi = ni + s_ref[0, chunk:chunk + 1, half:]
        starts_r.append(hr)
        starts_i.append(hi)
    start = (jnp.concatenate(starts_r, axis=0), jnp.concatenate(starts_i, axis=0))
    br = jnp.broadcast_to(ar, (CHUNKS, half))
    bi = jnp.broadcast_to(ai, (CHUNKS, half))

    def step(index, state):
        sr, si = state
        at = pl.ds(pl.multiple_of(index * CHUNKS, CHUNKS), CHUNKS)
        nr, ni = cmul(br, bi, sr, si)
        nr, ni = nr + work[at, :half], ni + work[at, half:]
        work[at, :half] = nr
        work[at, half:] = ni
        return nr, ni

    lax.fori_loop(0, rows // CHUNKS, step, start, unroll=8)
    mixed = jnp.dot(work[...].astype(BF16), c_ref[0], preferred_element_type=F32)
    mixed = mixed + k_ref[0] * x_ref[...].astype(F32)
    o_ref[...] = jax.nn.gelu(mixed).astype(BF16)


def exchange(sizes, e_ref, o_ref, send_sem, recv_sem):
    n = 1
    me = 0
    for name in SP:
        n *= sizes[name]
        me = me * sizes[name] + lax.axis_index(name)
    core = lax.axis_index("tp")

    def device(position):
        coords = []
        for name in reversed(SP):
            coords.append(lax.rem(position, sizes[name]))
            position = position // sizes[name]
        return (*reversed(coords), core)

    barrier = pltpu.get_barrier_semaphore()
    for k in range(1, n):
        pl.semaphore_signal(
            barrier, inc=1, device_id=device(lax.rem(me + k, n)),
            device_id_type=pl.DeviceIdType.MESH,
        )
    pl.semaphore_wait(barrier, n - 1)
    copies = []
    for k in range(1, n):
        copy = pltpu.make_async_remote_copy(
            src_ref=e_ref,
            dst_ref=o_ref.at[me],
            send_sem=send_sem.at[k],
            recv_sem=recv_sem.at[k],
            device_id=device(lax.rem(me + k, n)),
            device_id_type=pl.DeviceIdType.MESH,
        )
        copy.start()
        copies.append(copy)
    o_ref[me] = e_ref[...]
    for copy in copies:
        copy.wait()


def mixer(sizes, mixer_in, decay_real, decay_imag, log_step, in_real, in_imag,
          output_real, output_imaginary, skip):
    rows, channels = mixer_in.shape
    groups, states = decay_real.shape
    blocks = groups // GATHER
    cb, sb = channels // blocks, GATHER * states
    n = sizes["h"] * sizes["u"] * sizes["m"] * sizes["v"]
    power_re, power_im, bar_re, bar_im = discrete(
        decay_real, decay_imag, log_step, in_real, in_imag
    )
    swap = lambda t: jnp.transpose(t, (0, 2, 1))
    read_in = jnp.concatenate(
        [spread(swap(bar_re)), spread(swap(bar_im))], axis=2
    ).astype(BF16)
    read_out = jnp.concatenate(
        [spread(swap(output_real)), -spread(swap(output_imaginary))], axis=1
    ).astype(BF16)
    power = jnp.stack([power_re.reshape(blocks, sb), power_im.reshape(blocks, sb)], axis=1)
    span = rows // CHUNKS
    x = mixer_in.reshape(CHUNKS, span, channels).transpose(1, 0, 2).reshape(rows, channels)

    x_spec = pl.BlockSpec((rows, cb), lambda b: (0, b))
    whole = lambda *shape: pl.BlockSpec((1, *shape), lambda b: (b, 0, 0))
    ends, total = pl.pallas_call(
        scan_ends,
        grid=(blocks,),
        in_specs=[x_spec, whole(cb, 2 * sb), whole(2, sb)],
        out_specs=[whole(CHUNKS, 2 * sb), whole(1, 2 * sb)],
        out_shape=[
            jax.ShapeDtypeStruct((blocks, CHUNKS, 2 * sb), F32),
            jax.ShapeDtypeStruct((blocks, 1, 2 * sb), F32),
        ],
        scratch_shapes=[pltpu.VMEM((rows, 2 * sb), F32)],
        cost_estimate=pl.CostEstimate(
            flops=2 * rows * cb * sb * 2 * blocks, bytes_accessed=rows * channels * 4,
            transcendentals=0,
        ),
        name="scan_ends",
    )(x, read_in, power)

    lines = blocks * 2 * sb // 128
    gathered = pl.pallas_call(
        functools.partial(exchange, sizes),
        in_specs=[pl.BlockSpec(memory_space=pltpu.VMEM)],
        out_specs=pl.BlockSpec(memory_space=pltpu.VMEM),
        out_shape=jax.ShapeDtypeStruct((n, lines, 128), F32),
        scratch_shapes=[pltpu.SemaphoreType.DMA((n,)), pltpu.SemaphoreType.DMA((n,))],
        compiler_params=pltpu.CompilerParams(collective_id=0, has_side_effects=True),
        cost_estimate=pl.CostEstimate(
            flops=10**7, bytes_accessed=n * lines * 512, transcendentals=0
        ),
        name="exchange",
    )(total.reshape(lines, 128))
    gathered = gathered.reshape(n, blocks, 2 * sb).transpose(1, 0, 2)

    me = lax.axis_index(SP).astype(jnp.int32).reshape(1)
    activated = pl.pallas_call(
        scan_outputs,
        grid=(blocks,),
        in_specs=[
            pl.BlockSpec(memory_space=pltpu.SMEM),
            x_spec,
            whole(cb, 2 * sb),
            whole(2 * sb, cb),
            whole(2, sb),
            whole(CHUNKS, 2 * sb),
            whole(n, 2 * sb),
            whole(1, cb),
        ],
        out_specs=x_spec,
        out_shape=jax.ShapeDtypeStruct((rows, channels), BF16),
        scratch_shapes=[pltpu.VMEM((rows, 2 * sb), F32)],
        cost_estimate=pl.CostEstimate(
            flops=4 * rows * cb * sb * 2 * blocks, bytes_accessed=rows * channels * 4,
            transcendentals=rows * channels,
        ),
        name="scan_outputs",
    )(me, x, read_in, read_out, power, ends, gathered, skip.reshape(blocks, 1, cb))
    return activated.reshape(span, CHUNKS, channels).transpose(1, 0, 2).reshape(rows, channels)


def flip(value, axes, count, k):
    return lax.ppermute(value, axes, [(i, i ^ k) for i in range(count)])


def at(stack, index):
    return lax.dynamic_index_in_dim(stack, index, 0, keepdims=False)


def collect(sizes, quarters):
    h, m = sizes["h"], sizes["m"]
    mine = lax.axis_index(PEERS)
    ih, im = lax.axis_index("h"), lax.axis_index("m")
    block = jnp.zeros(quarters.shape, quarters.dtype)
    for k in range(4):
        piece = at(quarters, mine ^ k)
        if k:
            piece = flip(piece, PEERS, 4, k)
        block = lax.dynamic_update_index_in_dim(block, piece, mine ^ k, 0)
    tail = quarters.shape[1:]
    full = jnp.zeros((h, 2, m, 2, *tail), quarters.dtype)
    for r in range(h):
        there = block
        if r:
            there = lax.ppermute(block, "h", [(i, (i + r) % h) for i in range(h)])
        for s in range(m):
            got = there
            if s:
                got = lax.ppermute(there, "m", [(i, (i + s) % m) for i in range(m)])
            full = lax.dynamic_update_slice(
                full, got.reshape(1, 2, 1, 2, *tail),
                (lax.rem(ih - r + h, h), 0, lax.rem(im - s + m, m), 0, *([0] * len(tail))),
            )
    return full.reshape(h * 4 * m, *tail)


def on_device(sizes, mixer_in, residual, decay_real, decay_imag, log_step, in_real, in_imag,
              output_real, output_imaginary, skip, out_proj, norm_gain, w_gate, w_up, w_down):
    tp = sizes["tp"]
    width = residual.shape[1]
    depth, hidden_units = w_gate.shape
    part = hidden_units // 4
    by_quarter = lambda w: w.reshape(depth, 4, part).transpose(1, 0, 2)
    full_gate = collect(sizes, by_quarter(w_gate)).reshape(width, part)
    full_up = collect(sizes, by_quarter(w_up)).reshape(width, part)
    full_down = collect(sizes, w_down.reshape(4, part, depth))
    full_down = full_down.transpose(1, 0, 2).reshape(part, width)

    activated = mixer(sizes, mixer_in, decay_real, decay_imag, log_step, in_real, in_imag,
                      output_real, output_imaginary, skip)
    share = jnp.dot(activated, out_proj, preferred_element_type=F32).astype(BF16)
    mine = lax.axis_index("tp")
    share = share.reshape(tp, -1, width)
    mixed = at(share, mine).astype(F32)
    for t in range(1, tp):
        mixed = mixed + flip(at(share, mine ^ t), "tp", tp, t).astype(F32)
    mixed = mixed.astype(BF16)
    carried = residual.astype(F32) + mixed.astype(F32)
    scale = lax.rsqrt(jnp.mean(carried * carried, axis=-1, keepdims=True) + 1e-06)
    normed = (carried * scale * norm_gain).astype(BF16)

    rows = jnp.stack([normed] + [flip(normed, PEERS, 4, k) for k in range(1, 4)])
    rows = jnp.stack([rows] + [flip(rows, "tp", tp, t) for t in range(1, tp)])
    shape = rows.shape
    rows = rows.reshape(-1, width)
    gate = jnp.dot(rows, full_gate, preferred_element_type=F32)
    up = jnp.dot(rows, full_up, preferred_element_type=F32)
    hidden = (jax.nn.silu(gate) * up).astype(BF16)
    down = jnp.dot(hidden, full_down, preferred_element_type=F32).astype(BF16).reshape(shape)
    summed = down[0].astype(F32)
    for t in range(1, tp):
        summed = summed + flip(down[t], "tp", tp, t).astype(F32)
    summed = summed.astype(BF16)
    total = summed[0].astype(F32)
    for k in range(1, 4):
        total = total + flip(summed[k], PEERS, 4, k).astype(F32)
    total = total.astype(BF16)
    return (carried + 0.5 * total.astype(F32)).astype(BF16)


def solution(mesh):
    sp, tp = mesh.shape["sp"], mesh.shape["tp"]
    sizes = {"h": sp // 8, "u": 2, "m": 2, "v": 2, "tp": tp}
    cut = Mesh(mesh.devices.reshape(tuple(sizes.values())), tuple(sizes))
    return jax.shard_map(
        functools.partial(on_device, sizes),
        mesh=cut,
        in_specs=(
            P(SP, "tp"),
            P((*SP, "tp"), None),
            P("tp", None),
            P("tp", None),
            P("tp"),
            P("tp", None, None),
            P("tp", None, None),
            P("tp", None, None),
            P("tp", None, None),
            P("tp"),
            P("tp", None),
            P(),
            P(SP, "tp"),
            P(SP, "tp"),
            P("tp", SP),
        ),
        out_specs=P((*SP, "tp"), None),
        check_vma=False,
    )
```

```python
import functools

import jax
import jax.numpy as jnp
from jax import lax
from jax.experimental import pallas as pl
from jax.experimental.pallas import tpu as pltpu
from jax.sharding import Mesh
from jax.sharding import PartitionSpec as P

F32 = jnp.float32
BF16 = jnp.bfloat16
SP = ("h", "u", "m", "v")
PEERS = ("u", "v")
GATHER = 8
CHUNKS = 8
MESH = pl.DeviceIdType.MESH


def discrete(decay_real, decay_imag, log_step, in_real, in_imag):
    step_size = jnp.exp(log_step)[:, None]
    magnitude = jnp.exp(decay_real * step_size)
    angle = decay_imag * step_size
    power_re = magnitude * jnp.cos(angle)
    power_im = magnitude * jnp.sin(angle)
    denom = decay_real * decay_real + decay_imag * decay_imag
    ratio_re = ((power_re - 1.0) * decay_real + power_im * decay_imag) / denom
    ratio_im = (power_im * decay_real - (power_re - 1.0) * decay_imag) / denom
    drive_re = ratio_re[..., None] * in_real - ratio_im[..., None] * in_imag
    drive_im = ratio_re[..., None] * in_imag + ratio_im[..., None] * in_real
    return (power_re, power_im, drive_re, drive_im)


def cmul(ar, ai, br, bi):
    return ar * br - ai * bi, ar * bi + ai * br


def cpow(ar, ai, count):
    result = None
    while count:
        if count & 1:
            result = (ar, ai) if result is None else cmul(*result, ar, ai)
        count >>= 1
        if count:
            ar, ai = cmul(ar, ai, ar, ai)
    return result


def iota(shape, dim):
    return lax.broadcasted_iota(jnp.int32, shape, dim)


def tiled(block, copies, across, down):
    rows, columns = block.shape
    wide = (columns, columns * copies)
    pick = (iota(wide, 0) == lax.rem(iota(wide, 1), columns)).astype(BF16)
    full = jnp.dot(block, pick, preferred_element_type=F32)
    keep = lax.div(iota(full.shape, 0), down) == lax.div(iota(full.shape, 1), across)
    return jnp.where(keep, full, 0.0).astype(BF16)


def front(sizes, x_ref, b_ref, c_ref, a_ref, k_ref, wo_ref, res_ref, gain_ref, *rest):
    quarters, rest = rest[:3], rest[3:]
    weights, (rows_ref, carried_ref), rest = rest[:3], rest[3:5], rest[5:]
    (work, read_in, read_out, ends, total, gathered, act, share, others,
     send_sem, recv_sem, local_sem) = rest
    blocks, rows, cb = x_ref.shape
    sb = a_ref.shape[2]
    depth = quarters[0].shape[2]
    width = wo_ref.shape[1]
    span = rows // CHUNKS
    nh, nm, tp = sizes["h"], sizes["m"], sizes["tp"]
    n = nh * 4 * nm
    h, u, m, v, core = (lax.axis_index(name) for name in (*SP, "tp"))
    index = lambda h, u, m, v: ((h * 2 + u) * nm + m) * 2 + v
    me = index(h, u, m, v)
    peer = lambda k: (1 - u if k & 2 else u, 1 - v if k & 1 else v)
    counter = iter(range(send_sem.shape[0]))

    def send(src, dst, device):
        slot = next(counter)
        copy = pltpu.make_async_remote_copy(
            src_ref=src, dst_ref=dst, send_sem=send_sem.at[slot], recv_sem=recv_sem.at[slot],
            device_id=device, device_id_type=MESH,
        )
        copy.start()
        return copy

    def place(ref, position):
        if depth % 128:
            return ref.at[position]
        return ref.at[:, pl.ds(pl.multiple_of(position * depth, depth), depth)]

    barrier = pltpu.get_barrier_semaphore()
    others_sp = []
    for k in range(1, n):
        to = lax.rem(me + k, n)
        there = (lax.div(to, 4 * nm), lax.rem(lax.div(to, 2 * nm), 2),
                 lax.rem(lax.div(to, 2), nm), lax.rem(to, 2), core)
        others_sp.append(there)
        pl.semaphore_signal(barrier, inc=1, device_id=there, device_id_type=MESH)
    for t in range(1, tp):
        pl.semaphore_signal(
            barrier, inc=1, device_id=(h, u, m, v, lax.rem(core + t, tp)), device_id_type=MESH
        )
    pl.semaphore_wait(barrier, n - 1 + tp - 1)

    sent = []
    first = {}
    over_h = {}
    over_m = {}

    def spread_h(w, k, src, position):
        for r in range(1, nh):
            pu, pv = peer(k)
            copy = send(src, place(weights[w], position), (lax.rem(h + r, nh), u, m, v, core))
            over_h[w, k, r] = copy

    def spread_m(w, k, r, src, position):
        for s in range(1, nm):
            over_m[w, k, r, s] = send(
                src, place(weights[w], position), (h, u, lax.rem(m + s, nm), v, core)
            )

    own = u * 2 + v
    for w in range(3):
        for k in (3, 1, 2):
            pu, pv = peer(k)
            first[w, k] = send(
                quarters[w].at[pu * 2 + pv], place(weights[w], me), (h, pu, m, pv, core)
            )
    locals_ = []
    for w in range(3):
        spread_h(w, 0, quarters[w].at[own], me)
        spread_m(w, 0, 0, quarters[w].at[own], me)
        copy = pltpu.make_async_copy(quarters[w].at[own], place(weights[w], me), local_sem.at[w])
        copy.start()
        locals_.append(copy)

    def scan(b, start, keep):
        work[...] = jnp.dot(x_ref[b], read_in[b], preferred_element_type=F32)
        br = jnp.broadcast_to(a_ref[b, 0:1, :], (CHUNKS, sb))
        bi = jnp.broadcast_to(a_ref[b, 1:2, :], (CHUNKS, sb))

        def step(i, state):
            at = pl.ds(pl.multiple_of(i * CHUNKS, CHUNKS), CHUNKS)
            nr, ni = cmul(br, bi, *state)
            nr, ni = nr + work[at, :sb], ni + work[at, sb:]
            if keep:
                work[at, :sb] = nr
                work[at, sb:] = ni
            return nr, ni

        return lax.fori_loop(0, span, step, start, unroll=8)

    @pl.loop(0, blocks)
    def _(b):
        states = b_ref.shape[3]
        for half in range(2):
            read_in[b, :, half * sb:(half + 1) * sb] = tiled(
                b_ref[b, half], GATHER, states, cb // GATHER
            )
            read_out[b, half * sb:(half + 1) * sb, :] = tiled(
                c_ref[b, half], GATHER, cb // GATHER, states
            )
        zero = jnp.zeros((CHUNKS, sb), F32)
        sr, si = scan(b, (zero, zero), False)
        ends[b, :, :sb] = sr
        ends[b, :, sb:] = si
        lr, li = cpow(a_ref[b, 0:1, :], a_ref[b, 1:2, :], span)
        er, ei = sr[0:1], si[0:1]
        for chunk in range(1, CHUNKS):
            er, ei = cmul(lr, li, er, ei)
            er, ei = er + sr[chunk:chunk + 1], ei + si[chunk:chunk + 1]
        total[b, :, :sb] = er
        total[b, :, sb:] = ei

    states_out = [send(total, gathered.at[me], there) for there in others_sp]
    gathered[me] = total[...]
    for copy in states_out:
        copy.wait_recv()

    @pl.loop(0, blocks)
    def _(b):
        lr, li = cpow(a_ref[b, 0:1, :], a_ref[b, 1:2, :], span)
        tr, ti = cpow(lr, li, CHUNKS)
        hr = jnp.zeros((1, sb), F32)
        hi = hr
        for device in range(n - 1):
            nr, ni = cmul(tr, ti, hr, hi)
            nr = nr + gathered[device, b, :, :sb]
            ni = ni + gathered[device, b, :, sb:]
            hr, hi = jnp.where(device < me, nr, hr), jnp.where(device < me, ni, hi)
        starts_r, starts_i = [hr], [hi]
        for chunk in range(CHUNKS - 1):
            nr, ni = cmul(lr, li, hr, hi)
            hr = nr + ends[b, chunk:chunk + 1, :sb]
            hi = ni + ends[b, chunk:chunk + 1, sb:]
            starts_r.append(hr)
            starts_i.append(hi)
        scan(b, (jnp.concatenate(starts_r, axis=0), jnp.concatenate(starts_i, axis=0)), True)
        mixed = jnp.dot(work[...].astype(BF16), read_out[b], preferred_element_type=F32)
        mixed = mixed + k_ref[b] * x_ref[b].astype(F32)
        mixed = jax.nn.gelu(mixed).astype(BF16)
        square = (rows, rows)
        source = lax.rem(iota(square, 0), span) * CHUNKS + lax.div(iota(square, 0), span)
        turn = (iota(square, 1) == source).astype(BF16)
        act[:, pl.ds(pl.multiple_of(b * cb, cb), cb)] = jnp.dot(
            turn, mixed, preferred_element_type=F32
        ).astype(BF16)

    keep_rows = rows // tp
    tile = min(512, width)
    mixed_copies = []
    for t in (*range(1, tp), 0):
        to = lax.rem(core + t, tp)

        @pl.loop(0, width // tile)
        def _(j):
            at = pl.ds(pl.multiple_of(j * tile, tile), tile)
            share[t, :, at] = jnp.dot(
                act[pl.ds(pl.multiple_of(to * keep_rows, keep_rows), keep_rows), :],
                wo_ref[:, at], preferred_element_type=F32,
            ).astype(BF16)

        if t:
            mixed_copies.append(send(share.at[t], others.at[t - 1], (h, u, m, v, to)))

    for w in range(3):
        for k in (1, 2, 3):
            first[w, k].wait_recv()
            pu, pv = peer(k)
            position = index(h, pu, m, pv)
            spread_h(w, k, place(weights[w], position), position)
            spread_m(w, k, 0, place(weights[w], position), position)

    for copy in mixed_copies:
        copy.wait_recv()
    line = min(32, keep_rows)

    @pl.loop(0, keep_rows // line)
    def _(i):
        at = pl.ds(pl.multiple_of(i * line, line), line)
        mixed = share[0, at, :].astype(F32)
        for t in range(1, tp):
            mixed = mixed + others[t - 1, at, :].astype(F32)
        carried = res_ref[at, :].astype(F32) + mixed.astype(BF16).astype(F32)
        scale = lax.rsqrt(jnp.mean(carried * carried, axis=-1, keepdims=True) + 1e-06)
        carried_ref[at, :] = carried
        rows_ref[0, 0, at, :] = (carried * scale * gain_ref[...]).astype(BF16)

    row_copies = {}
    for k in (3, 1, 2):
        pu, pv = peer(k)
        row_copies[k] = send(rows_ref.at[0, 0], rows_ref.at[0, k], (h, pu, m, pv, core))
    last = []
    for t in range(1, tp):
        last.append(send(rows_ref.at[0, 0], rows_ref.at[t, 0], (h, u, m, v, lax.rem(core + t, tp))))

    def pass_m(w, k):
        pu, pv = peer(k)
        for r in range(1, nh):
            over_h[w, k, r].wait_recv()
            position = index(lax.rem(h - r + nh, nh), pu, m, pv)
            spread_m(w, k, r, place(weights[w], position), position)

    for w in range(3):
        for k in range(4):
            pass_m(w, k)
        if w == 1:
            for k in (1, 2, 3):
                row_copies[k].wait_recv()
                for t in range(1, tp):
                    last.append(send(
                        rows_ref.at[0, k], rows_ref.at[t, k], (h, u, m, v, lax.rem(core + t, tp))
                    ))
    for copy in (*over_m.values(), *last):
        copy.wait_recv()
    for copy in (*first.values(), *over_h.values(), *over_m.values(), *states_out,
                 *mixed_copies, *row_copies.values(), *last):
        copy.wait_send()
    for copy in locals_:
        copy.wait()


def shift(value, axis, count, by):
    return lax.ppermute(value, axis, [(i, (i + by) % count) for i in range(count)])


def flip(value, axes, count, k):
    return lax.ppermute(value, axes, [(i, i ^ k) for i in range(count)])


def on_device(sizes, mixer_in, residual, decay_real, decay_imag, log_step, in_real, in_imag,
              output_real, output_imaginary, skip, out_proj, norm_gain, w_gate, w_up, w_down):
    tp, nh, nm = sizes["tp"], sizes["h"], sizes["m"]
    n = nh * 4 * nm
    rows, channels = mixer_in.shape
    keep_rows, width = residual.shape
    depth, hidden_units = w_gate.shape
    part = hidden_units // 4
    groups, states = decay_real.shape
    blocks = groups // GATHER
    cb, sb = channels // blocks, GATHER * states
    power_re, power_im, bar_re, bar_im = discrete(
        decay_real, decay_imag, log_step, in_real, in_imag
    )
    rows_first = lambda t: jnp.transpose(t, (0, 2, 1)).reshape(blocks, -1, t.shape[1])
    read_in = jnp.stack([rows_first(bar_re), rows_first(bar_im)], axis=1).astype(BF16)
    read_out = jnp.stack(
        [rows_first(output_real), -rows_first(output_imaginary)], axis=1
    ).astype(BF16)
    power = jnp.stack([power_re.reshape(blocks, sb), power_im.reshape(blocks, sb)], axis=1)
    x = mixer_in.reshape(CHUNKS, rows // CHUNKS, blocks, cb).transpose(2, 1, 0, 3)
    x = x.reshape(blocks, rows, cb)
    copies = 3 * (3 + 4 * (nh - 1) + 4 * nh * (nm - 1)) + (n - 1) + (tp - 1) + 3 + 4 * (tp - 1)
    laid = (part, n * depth) if depth % 128 == 0 else (n, part, depth)
    vmem = pl.BlockSpec(memory_space=pltpu.VMEM)
    full_gate, full_up, full_down, rows_all, carried = pl.pallas_call(
        functools.partial(front, sizes),
        in_specs=[vmem] * 11,
        out_specs=[vmem] * 5,
        out_shape=[jax.ShapeDtypeStruct(laid, BF16)] * 3 + [
            jax.ShapeDtypeStruct((tp, 4, keep_rows, width), BF16),
            jax.ShapeDtypeStruct((keep_rows, width), F32),
        ],
        scratch_shapes=[
            pltpu.VMEM((rows, 2 * sb), F32),
            pltpu.VMEM((blocks, cb, 2 * sb), BF16),
            pltpu.VMEM((blocks, 2 * sb, cb), BF16),
            pltpu.VMEM((blocks, CHUNKS, 2 * sb), F32),
            pltpu.VMEM((blocks, 1, 2 * sb), F32),
            pltpu.VMEM((n, blocks, 1, 2 * sb), F32),
            pltpu.VMEM((rows, channels), BF16),
            pltpu.VMEM((tp, keep_rows, width), BF16),
            pltpu.VMEM((tp - 1, keep_rows, width), BF16),
            pltpu.SemaphoreType.DMA((copies,)),
            pltpu.SemaphoreType.DMA((copies,)),
            pltpu.SemaphoreType.DMA((3,)),
        ],
        compiler_params=pltpu.CompilerParams(
            collective_id=0, has_side_effects=True, vmem_limit_bytes=60 * 2**20
        ),
        name="front",
    )(x, read_in, read_out, power, skip.reshape(blocks, 1, cb), out_proj, residual,
      norm_gain.reshape(1, width), w_gate.T.reshape(4, part, depth),
      w_up.T.reshape(4, part, depth), w_down.reshape(4, part, depth))
    if len(laid) == 3:
        full_gate, full_up, full_down = (
            t.transpose(1, 0, 2).reshape(part, width) for t in (full_gate, full_up, full_down)
        )

    flat = rows_all.reshape(-1, width)
    across = (((1,), (1,)), ((), ()))
    gate = lax.dot_general(flat, full_gate, across, preferred_element_type=F32)
    up = lax.dot_general(flat, full_up, across, preferred_element_type=F32)
    hidden = (jax.nn.silu(gate) * up).astype(BF16)
    down = jnp.dot(hidden, full_down, preferred_element_type=F32).astype(BF16)
    down = down.reshape(rows_all.shape)
    summed = down[0].astype(F32)
    for t in range(1, tp):
        summed = summed + shift(down[t], "tp", tp, -t).astype(F32)
    summed = summed.astype(BF16)
    total = summed[0].astype(F32)
    for k in range(1, 4):
        total = total + flip(summed[k], PEERS, 4, k).astype(F32)
    total = total.astype(BF16)
    return (carried + 0.5 * total.astype(F32)).astype(BF16)


def solution(mesh):
    sp, tp = mesh.shape["sp"], mesh.shape["tp"]
    sizes = {"h": sp // 8, "u": 2, "m": 2, "v": 2, "tp": tp}
    cut = Mesh(mesh.devices.reshape(tuple(sizes.values())), tuple(sizes))
    return jax.shard_map(
        functools.partial(on_device, sizes),
        mesh=cut,
        in_specs=(
            P(SP, "tp"),
            P((*SP, "tp"), None),
            P("tp", None),
            P("tp", None),
            P("tp"),
            P("tp", None, None),
            P("tp", None, None),
            P("tp", None, None),
            P("tp", None, None),
            P("tp"),
            P("tp", None),
            P(),
            P(SP, "tp"),
            P(SP, "tp"),
            P("tp", SP),
        ),
        out_specs=P((*SP, "tp"), None),
        check_vma=False,
    )
```

```python
import functools

import jax
import jax.numpy as jnp
from jax import lax
from jax.experimental import pallas as pl
from jax.experimental.pallas import tpu as pltpu
from jax.sharding import Mesh
from jax.sharding import PartitionSpec as P

F32 = jnp.float32
BF16 = jnp.bfloat16
SP = ("h", "u", "m", "v")
PEERS = ("u", "v")
GATHER = 8
CHUNKS = 8
MESH = pl.DeviceIdType.MESH


def discrete(decay_real, decay_imag, log_step, in_real, in_imag):
    step_size = jnp.exp(log_step)[:, None]
    magnitude = jnp.exp(decay_real * step_size)
    angle = decay_imag * step_size
    power_re = magnitude * jnp.cos(angle)
    power_im = magnitude * jnp.sin(angle)
    denom = decay_real * decay_real + decay_imag * decay_imag
    ratio_re = ((power_re - 1.0) * decay_real + power_im * decay_imag) / denom
    ratio_im = (power_im * decay_real - (power_re - 1.0) * decay_imag) / denom
    drive_re = ratio_re[..., None] * in_real - ratio_im[..., None] * in_imag
    drive_im = ratio_re[..., None] * in_imag + ratio_im[..., None] * in_real
    return (power_re, power_im, drive_re, drive_im)


def cmul(ar, ai, br, bi):
    return ar * br - ai * bi, ar * bi + ai * br


def cpow(ar, ai, count):
    result = None
    while count:
        if count & 1:
            result = (ar, ai) if result is None else cmul(*result, ar, ai)
        count >>= 1
        if count:
            ar, ai = cmul(ar, ai, ar, ai)
    return result


def iota(shape, dim):
    return lax.broadcasted_iota(jnp.int32, shape, dim)


def tiled(block, copies, across, down):
    rows, columns = block.shape
    wide = (columns, columns * copies)
    pick = (iota(wide, 0) == lax.rem(iota(wide, 1), columns)).astype(BF16)
    full = jnp.dot(block, pick, preferred_element_type=F32)
    keep = lax.div(iota(full.shape, 0), down) == lax.div(iota(full.shape, 1), across)
    return jnp.where(keep, full, 0.0).astype(BF16)


def layer(sizes, fused, x_ref, b_ref, c_ref, a_ref, k_ref, wo_ref, res_ref, gain_ref, *rest):
    quarters, rest = rest[:3], rest[3:]
    if fused:
        out_ref, *rest = rest
        hidden, partners, peers, *rest = rest
    weights, (rows_ref, carried_ref), rest = rest[:3], rest[3:5], rest[5:]
    (work, read_in, read_out, ends, total, gathered, act, share, others,
     send_sem, recv_sem, local_sem) = rest
    blocks, rows, cb = x_ref.shape
    sb = a_ref.shape[2]
    depth = quarters[0].shape[2]
    width = wo_ref.shape[1]
    span = rows // CHUNKS
    nh, nm, tp = sizes["h"], sizes["m"], sizes["tp"]
    n = nh * 4 * nm
    h, u, m, v, core = (lax.axis_index(name) for name in (*SP, "tp"))
    index = lambda h, u, m, v: ((h * 2 + u) * nm + m) * 2 + v
    me = index(h, u, m, v)
    peer = lambda k: (1 - u if k & 2 else u, 1 - v if k & 1 else v)
    counter = iter(range(send_sem.shape[0]))

    def send(src, dst, device):
        slot = next(counter)
        copy = pltpu.make_async_remote_copy(
            src_ref=src, dst_ref=dst, send_sem=send_sem.at[slot], recv_sem=recv_sem.at[slot],
            device_id=device, device_id_type=MESH,
        )
        copy.start()
        return copy

    def place(ref, position):
        if depth % 128:
            return ref.at[position]
        return ref.at[:, pl.ds(pl.multiple_of(position * depth, depth), depth)]

    barrier = pltpu.get_barrier_semaphore()
    others_sp = []
    for k in range(1, n):
        to = lax.rem(me + k, n)
        there = (lax.div(to, 4 * nm), lax.rem(lax.div(to, 2 * nm), 2),
                 lax.rem(lax.div(to, 2), nm), lax.rem(to, 2), core)
        others_sp.append(there)
        pl.semaphore_signal(barrier, inc=1, device_id=there, device_id_type=MESH)
    for t in range(1, tp):
        pl.semaphore_signal(
            barrier, inc=1, device_id=(h, u, m, v, lax.rem(core + t, tp)), device_id_type=MESH
        )
    pl.semaphore_wait(barrier, n - 1 + tp - 1)

    sent = []
    first = {}
    over_h = {}
    over_m = {}

    def spread_h(w, k, src, position):
        for r in range(1, nh):
            pu, pv = peer(k)
            copy = send(src, place(weights[w], position), (lax.rem(h + r, nh), u, m, v, core))
            over_h[w, k, r] = copy

    def spread_m(w, k, r, src, position):
        for s in range(1, nm):
            over_m[w, k, r, s] = send(
                src, place(weights[w], position), (h, u, lax.rem(m + s, nm), v, core)
            )

    own = u * 2 + v
    for w in range(3):
        for k in (3, 1, 2):
            pu, pv = peer(k)
            first[w, k] = send(
                quarters[w].at[pu * 2 + pv], place(weights[w], me), (h, pu, m, pv, core)
            )
    locals_ = []
    for w in range(3):
        spread_h(w, 0, quarters[w].at[own], me)
        spread_m(w, 0, 0, quarters[w].at[own], me)
        copy = pltpu.make_async_copy(quarters[w].at[own], place(weights[w], me), local_sem.at[w])
        copy.start()
        locals_.append(copy)

    def scan(b, start, keep):
        work[...] = jnp.dot(x_ref[b], read_in[b], preferred_element_type=F32)
        br = jnp.broadcast_to(a_ref[b, 0:1, :], (CHUNKS, sb))
        bi = jnp.broadcast_to(a_ref[b, 1:2, :], (CHUNKS, sb))

        def step(i, state):
            at = pl.ds(pl.multiple_of(i * CHUNKS, CHUNKS), CHUNKS)
            nr, ni = cmul(br, bi, *state)
            nr, ni = nr + work[at, :sb], ni + work[at, sb:]
            if keep:
                work[at, :sb] = nr
                work[at, sb:] = ni
            return nr, ni

        return lax.fori_loop(0, span, step, start, unroll=8)

    @pl.loop(0, blocks)
    def _(b):
        states = b_ref.shape[3]
        for half in range(2):
            read_in[b, :, half * sb:(half + 1) * sb] = tiled(
                b_ref[b, half], GATHER, states, cb // GATHER
            )
            read_out[b, half * sb:(half + 1) * sb, :] = tiled(
                c_ref[b, half], GATHER, cb // GATHER, states
            )
        zero = jnp.zeros((CHUNKS, sb), F32)
        sr, si = scan(b, (zero, zero), False)
        ends[b, :, :sb] = sr
        ends[b, :, sb:] = si
        lr, li = cpow(a_ref[b, 0:1, :], a_ref[b, 1:2, :], span)
        er, ei = sr[0:1], si[0:1]
        for chunk in range(1, CHUNKS):
            er, ei = cmul(lr, li, er, ei)
            er, ei = er + sr[chunk:chunk + 1], ei + si[chunk:chunk + 1]
        total[b, :, :sb] = er
        total[b, :, sb:] = ei

    states_out = [send(total, gathered.at[me], there) for there in others_sp]
    gathered[me] = total[...]
    for copy in states_out:
        copy.wait_recv()

    @pl.loop(0, blocks)
    def _(b):
        lr, li = cpow(a_ref[b, 0:1, :], a_ref[b, 1:2, :], span)
        tr, ti = cpow(lr, li, CHUNKS)
        hr = jnp.zeros((1, sb), F32)
        hi = hr
        for device in range(n - 1):
            nr, ni = cmul(tr, ti, hr, hi)
            nr = nr + gathered[device, b, :, :sb]
            ni = ni + gathered[device, b, :, sb:]
            hr, hi = jnp.where(device < me, nr, hr), jnp.where(device < me, ni, hi)
        starts_r, starts_i = [hr], [hi]
        for chunk in range(CHUNKS - 1):
            nr, ni = cmul(lr, li, hr, hi)
            hr = nr + ends[b, chunk:chunk + 1, :sb]
            hi = ni + ends[b, chunk:chunk + 1, sb:]
            starts_r.append(hr)
            starts_i.append(hi)
        scan(b, (jnp.concatenate(starts_r, axis=0), jnp.concatenate(starts_i, axis=0)), True)
        mixed = jnp.dot(work[...].astype(BF16), read_out[b], preferred_element_type=F32)
        mixed = mixed + k_ref[b] * x_ref[b].astype(F32)
        mixed = jax.nn.gelu(mixed).astype(BF16)
        square = (rows, rows)
        source = lax.rem(iota(square, 0), span) * CHUNKS + lax.div(iota(square, 0), span)
        turn = (iota(square, 1) == source).astype(BF16)
        act[:, pl.ds(pl.multiple_of(b * cb, cb), cb)] = jnp.dot(
            turn, mixed, preferred_element_type=F32
        ).astype(BF16)

    keep_rows = rows // tp
    tile = min(512, width)
    mixed_copies = []
    for t in (*range(1, tp), 0):
        to = lax.rem(core + t, tp)

        @pl.loop(0, width // tile)
        def _(j):
            at = pl.ds(pl.multiple_of(j * tile, tile), tile)
            share[t, :, at] = jnp.dot(
                act[pl.ds(pl.multiple_of(to * keep_rows, keep_rows), keep_rows), :],
                wo_ref[:, at], preferred_element_type=F32,
            ).astype(BF16)

        if t:
            mixed_copies.append(send(share.at[t], others.at[t - 1], (h, u, m, v, to)))

    for w in range(3):
        for k in (1, 2, 3):
            first[w, k].wait_recv()
            pu, pv = peer(k)
            position = index(h, pu, m, pv)
            spread_h(w, k, place(weights[w], position), position)
            spread_m(w, k, 0, place(weights[w], position), position)

    for copy in mixed_copies:
        copy.wait_recv()
    line = min(32, keep_rows)

    @pl.loop(0, keep_rows // line)
    def _(i):
        at = pl.ds(pl.multiple_of(i * line, line), line)
        mixed = share[0, at, :].astype(F32)
        for t in range(1, tp):
            mixed = mixed + others[t - 1, at, :].astype(F32)
        carried = res_ref[at, :].astype(F32) + mixed.astype(BF16).astype(F32)
        scale = lax.rsqrt(jnp.mean(carried * carried, axis=-1, keepdims=True) + 1e-06)
        carried_ref[at, :] = carried
        rows_ref[0, 0, at, :] = (carried * scale * gain_ref[...]).astype(BF16)

    row_copies = {}
    for k in (3, 1, 2):
        pu, pv = peer(k)
        row_copies[k] = send(rows_ref.at[0, 0], rows_ref.at[0, k], (h, pu, m, pv, core))
    last = []
    for t in range(1, tp):
        last.append(send(rows_ref.at[0, 0], rows_ref.at[t, 0], (h, u, m, v, lax.rem(core + t, tp))))

    def pass_m(w, k):
        pu, pv = peer(k)
        for r in range(1, nh):
            over_h[w, k, r].wait_recv()
            position = index(lax.rem(h - r + nh, nh), pu, m, pv)
            spread_m(w, k, r, place(weights[w], position), position)

    for w in range(3):
        for k in range(4):
            pass_m(w, k)
        if w == 1:
            for k in (1, 2, 3):
                row_copies[k].wait_recv()
                for t in range(1, tp):
                    last.append(send(
                        rows_ref.at[0, k], rows_ref.at[t, k], (h, u, m, v, lax.rem(core + t, tp))
                    ))
    sent = [*first.values(), *over_h.values(), *over_m.values(), *states_out, *mixed_copies]
    row_sends = [*row_copies.values(), *last]
    for (w, *_), copy in over_m.items():
        if w < 2 or not fused:
            copy.wait_recv()
    for copy in last:
        copy.wait_recv()
    for copy in locals_:
        copy.wait()
    if fused:
        sent += back(
            sizes, send, peer, (h, u, m, v, core), weights, rows_ref, carried_ref, out_ref,
            hidden, partners, peers, row_sends, [c for (w, *_), c in over_m.items() if w == 2],
        )
    else:
        sent += row_sends
    for copy in sent:
        copy.wait_send()


def back(sizes, send, peer, here, weights, rows_ref, carried_ref, out_ref, hidden, partners,
         peers, row_sends, down_copies):
    tp = sizes["tp"]
    h, u, m, v, core = here
    _, _, keep_rows, width = rows_ref.shape
    across = (((1,), (1,)), ((), ()))

    @pl.loop(0, 4 * tp)
    def _(i):
        t, k = lax.div(i, 4), lax.rem(i, 4)
        block = rows_ref[t, k]
        gate = lax.dot_general(block, weights[0][...], across, preferred_element_type=F32)
        up = lax.dot_general(block, weights[1][...], across, preferred_element_type=F32)
        hidden[i] = (jax.nn.silu(gate) * up).astype(BF16)

    for copy in (*down_copies,):
        copy.wait_recv()
    for copy in row_sends:
        copy.wait_send()

    tile = min(512, width)
    line = min(32, keep_rows)
    sent = []
    peer_copies = []
    from_core = {}

    def reduce(k):
        for copy in from_core[k]:
            copy.wait_recv()

        @pl.loop(0, keep_rows // line)
        def _(i):
            at = pl.ds(pl.multiple_of(i * line, line), line)
            total = rows_ref[0, k, at, :].astype(F32)
            for t in range(1, tp):
                total = total + partners[k, t - 1, at, :].astype(F32)
            rows_ref[0, k, at, :] = total.astype(BF16)

        if k:
            pu, pv = peer(k)
            peer_copies.append(send(rows_ref.at[0, k], peers.at[k - 1], (h, pu, m, pv, core)))

    order = (3, 1, 2, 0)
    for step, k in enumerate(order):
        from_core[k] = []
        for t in (*range(1, tp), 0):
            @pl.loop(0, width // tile)
            def _(j):
                at = pl.ds(pl.multiple_of(j * tile, tile), tile)
                rows_ref[t, k, :, at] = jnp.dot(
                    hidden[t * 4 + k], weights[2][:, at], preferred_element_type=F32
                ).astype(BF16)

            if t:
                from_core[k].append(send(
                    rows_ref.at[t, k], partners.at[k, t - 1],
                    (h, u, m, v, lax.rem(core + tp - t, tp)),
                ))
        reduce(k)
        sent += from_core[k]
    for copy in peer_copies:
        copy.wait_recv()

    @pl.loop(0, keep_rows // line)
    def _(i):
        at = pl.ds(pl.multiple_of(i * line, line), line)
        total = rows_ref[0, 0, at, :].astype(F32)
        for k in range(1, 4):
            total = total + peers[k - 1, at, :].astype(F32)
        total = total.astype(BF16).astype(F32)
        out_ref[at, :] = (carried_ref[at, :] + 0.5 * total).astype(BF16)

    return sent + peer_copies


def shift(value, axis, count, by):
    return lax.ppermute(value, axis, [(i, (i + by) % count) for i in range(count)])


def flip(value, axes, count, k):
    return lax.ppermute(value, axes, [(i, i ^ k) for i in range(count)])


def on_device(sizes, mixer_in, residual, decay_real, decay_imag, log_step, in_real, in_imag,
              output_real, output_imaginary, skip, out_proj, norm_gain, w_gate, w_up, w_down):
    tp, nh, nm = sizes["tp"], sizes["h"], sizes["m"]
    n = nh * 4 * nm
    rows, channels = mixer_in.shape
    keep_rows, width = residual.shape
    depth, hidden_units = w_gate.shape
    part = hidden_units // 4
    groups, states = decay_real.shape
    blocks = groups // GATHER
    cb, sb = channels // blocks, GATHER * states
    power_re, power_im, bar_re, bar_im = discrete(
        decay_real, decay_imag, log_step, in_real, in_imag
    )
    rows_first = lambda t: jnp.transpose(t, (0, 2, 1)).reshape(blocks, -1, t.shape[1])
    read_in = jnp.stack([rows_first(bar_re), rows_first(bar_im)], axis=1).astype(BF16)
    read_out = jnp.stack(
        [rows_first(output_real), -rows_first(output_imaginary)], axis=1
    ).astype(BF16)
    power = jnp.stack([power_re.reshape(blocks, sb), power_im.reshape(blocks, sb)], axis=1)
    x = mixer_in.reshape(CHUNKS, rows // CHUNKS, blocks, cb).transpose(2, 1, 0, 3)
    x = x.reshape(blocks, rows, cb)
    copies = 3 * (3 + 4 * (nh - 1) + 4 * nh * (nm - 1)) + (n - 1) + (tp - 1) + 3 + 4 * (tp - 1)
    laid = (part, n * depth) if depth % 128 == 0 else (n, part, depth)
    vmem = pl.BlockSpec(memory_space=pltpu.VMEM)
    between = [(laid, BF16)] * 3 + [
        ((tp, 4, keep_rows, width), BF16), ((keep_rows, width), F32),
    ]
    fused = depth % 128 == 0
    if fused:
        copies += 4 * (tp - 1) + 3
        out_shape = [jax.ShapeDtypeStruct((keep_rows, width), BF16)]
        extra = [
            pltpu.VMEM((4 * tp, keep_rows, part), BF16),
            pltpu.VMEM((4, tp - 1, keep_rows, width), BF16),
            pltpu.VMEM((3, keep_rows, width), BF16),
            *(pltpu.VMEM(*item) for item in between),
        ]
    else:
        out_shape = [jax.ShapeDtypeStruct(*item) for item in between]
        extra = []
    results = pl.pallas_call(
        functools.partial(layer, sizes, fused),
        in_specs=[vmem] * 11,
        out_specs=[vmem] * len(out_shape),
        out_shape=out_shape,
        scratch_shapes=[
            *extra,
            pltpu.VMEM((rows, 2 * sb), F32),
            pltpu.VMEM((blocks, cb, 2 * sb), BF16),
            pltpu.VMEM((blocks, 2 * sb, cb), BF16),
            pltpu.VMEM((blocks, CHUNKS, 2 * sb), F32),
            pltpu.VMEM((blocks, 1, 2 * sb), F32),
            pltpu.VMEM((n, blocks, 1, 2 * sb), F32),
            pltpu.VMEM((rows, channels), BF16),
            pltpu.VMEM((tp, keep_rows, width), BF16),
            pltpu.VMEM((tp - 1, keep_rows, width), BF16),
            pltpu.SemaphoreType.DMA((copies,)),
            pltpu.SemaphoreType.DMA((copies,)),
            pltpu.SemaphoreType.DMA((3,)),
        ],
        compiler_params=pltpu.CompilerParams(
            collective_id=0, has_side_effects=True, vmem_limit_bytes=62 * 2**20
        ),
        name="layer",
    )(x, read_in, read_out, power, skip.reshape(blocks, 1, cb), out_proj, residual,
      norm_gain.reshape(1, width), w_gate.T.reshape(4, part, depth),
      w_up.T.reshape(4, part, depth), w_down.reshape(4, part, depth))
    if fused:
        return results[0]
    full_gate, full_up, full_down, rows_all, carried = results
    if len(laid) == 3:
        full_gate, full_up, full_down = (
            t.transpose(1, 0, 2).reshape(part, width) for t in (full_gate, full_up, full_down)
        )

    flat = rows_all.reshape(-1, width)
    across = (((1,), (1,)), ((), ()))
    gate = lax.dot_general(flat, full_gate, across, preferred_element_type=F32)
    up = lax.dot_general(flat, full_up, across, preferred_element_type=F32)
    hidden = (jax.nn.silu(gate) * up).astype(BF16)
    down = jnp.dot(hidden, full_down, preferred_element_type=F32).astype(BF16)
    down = down.reshape(rows_all.shape)
    summed = down[0].astype(F32)
    for t in range(1, tp):
        summed = summed + shift(down[t], "tp", tp, -t).astype(F32)
    summed = summed.astype(BF16)
    total = summed[0].astype(F32)
    for k in range(1, 4):
        total = total + flip(summed[k], PEERS, 4, k).astype(F32)
    total = total.astype(BF16)
    return (carried + 0.5 * total.astype(F32)).astype(BF16)


def solution(mesh):
    sp, tp = mesh.shape["sp"], mesh.shape["tp"]
    sizes = {"h": sp // 8, "u": 2, "m": 2, "v": 2, "tp": tp}
    cut = Mesh(mesh.devices.reshape(tuple(sizes.values())), tuple(sizes))
    return jax.shard_map(
        functools.partial(on_device, sizes),
        mesh=cut,
        in_specs=(
            P(SP, "tp"),
            P((*SP, "tp"), None),
            P("tp", None),
            P("tp", None),
            P("tp"),
            P("tp", None, None),
            P("tp", None, None),
            P("tp", None, None),
            P("tp", None, None),
            P("tp"),
            P("tp", None),
            P(),
            P(SP, "tp"),
            P(SP, "tp"),
            P("tp", SP),
        ),
        out_specs=P((*SP, "tp"), None),
        check_vma=False,
    )
```
